32 devices in a mesh: sp: 8 (over z, x), tp: 4 (over y, core).
Axes of the slice: x: 2, y: 2, z: 4, core: 2. Of those that a mesh axis runs over, the one named last changes fastest.
Arguments:
- residual_in: bfloat16 [2048, 2048], P(('sp', 'tp')), may hold values from -6 to 6
- queries: bfloat16 [2048, 512], P('sp', 'tp'), may hold values from -6 to 6
- key_rows: bfloat16 [2048, 512], P('sp', 'tp'), may hold values from -6 to 6
- value_rows: bfloat16 [2048, 1024], P('sp', 'tp'), may hold values from -6 to 6
- out_gate: bfloat16 [2048, 1024], P('sp', 'tp'), may hold values from -6 to 6
- decay_logit: float32 [2048, 512], P('sp', 'tp'), may hold values from -30 to 30
- head_gain: bfloat16 [128], replicated, may hold values from 0.099609375 to 1.8984375
- w_out: bfloat16 [1024, 2048], replicated, may hold values from -0.1875 to 0.1875
- ffn_gain: bfloat16 [2048], replicated, may hold values from 0.099609375 to 1.8984375
- routing: int32 [2048, 4], P('sp'), may hold values from 0 to 7, all different within a row; in each aligned block of 64 rows (0 to 63, 64 to 127, ...) at most 64 rows name the same one
- route_weight: float32 [2048, 4], P(('sp', 'tp')), may hold values from 0.05 to 0.6
- w_gate: bfloat16 [8, 2048, 2048], P('sp', None, 'tp'), may hold values from -4 to 4
- w_up: bfloat16 [8, 2048, 2048], P('sp', None, 'tp'), may hold values from -4 to 4
- w_down: bfloat16 [8, 2048, 2048], P('sp', 'tp'), may hold values from -0.125 to 0.125
Outputs:
- layer_out: bfloat16 [2048, 2048], P(('sp', 'tp'))
The draws below stay inside these ranges and needn't reach their ends.
Inputs may be any that keep to these rules, and one draw needn't show every extreme that they name: `routing`: each row names 4 different experts. In each aligned block of 64 rows no expert is named more than 64 times, a bound that some blocks reach.
All inputs are finite; a program needn't handle non-finite values.
Results may differ from the reference program's by a relative error of at most 0.03.
Values may be sent and summed in bfloat16 or wider, within the bound.
A program may use at most 128 MiB of HBM per device.

```python
import math
import jax
import jax.numpy as jnp
import numpy as np
from jax import lax

D = 2048
HEADS = 8
DK = 64
DV = 128
FF = 2048
TOP = 4
BLOCK = 64
TOK_DEV = 256
TOKEN_COUNT = 2048
EXPERTS = 8
QROWS = 64
CAP = 64
N_TP = 4


def draw_decay_logit(key, part):
    random_subkeys = jax.random.split(jax.random.fold_in(key, 31), 7)
    channels = HEADS * DK
    share_fast = 0.5
    fast_head = jax.random.uniform(random_subkeys[0], (HEADS,)) < share_fast
    fast_channel = jnp.repeat(fast_head, DK)
    fast_rate = jnp.exp(jax.random.uniform(random_subkeys[1], (channels,), minval=jnp.log(1.0 / 50.0), maxval=jnp.log(1.0 / 15.0)))
    slow_rate = jnp.exp(jax.random.uniform(random_subkeys[2], (channels,), minval=jnp.log(0.3), maxval=0.0)) * 0.7 / TOKEN_COUNT
    base_rate = jnp.where(fast_channel, fast_rate, slow_rate)
    span_count = TOKEN_COUNT // TOK_DEV
    span_factor = jnp.repeat(jnp.exp(jax.random.uniform(random_subkeys[3], (span_count,), minval=jnp.log(0.5), maxval=jnp.log(2.0))), TOK_DEV)
    jitter = jnp.exp(0.6 * jax.random.truncated_normal(random_subkeys[4], -3.0, 3.0, (TOKEN_COUNT, channels)))
    stepwise_results = base_rate[None, :] * span_factor[:, None] * jitter
    spike_location = jax.random.randint(random_subkeys[5], (3,), 0, TOKEN_COUNT)
    spike_penalty = jax.random.uniform(random_subkeys[6], (3,), minval=0.2, maxval=0.45)
    position_indices = jnp.arange(TOKEN_COUNT)
    spike_increment = jnp.sum(jnp.where(position_indices[:, None] == spike_location[None, :], -jnp.log(1.0 - spike_penalty)[None, :], 0.0), axis=1)
    stepwise_results = stepwise_results + spike_increment[:, None]
    scaled = 16.0 * stepwise_results
    return -jnp.log(jnp.expm1(scaled))


def column_scaled(key, salt_value):
    random_subkeys = jax.random.split(jax.random.fold_in(key, salt_value), 2)
    lowest = 0.3
    highest = 2.5
    scales = jnp.exp(jax.random.uniform(random_subkeys[0], (EXPERTS, 1, FF), minval=jnp.log(lowest), maxval=jnp.log(highest)))
    entries = jax.random.truncated_normal(random_subkeys[1], -4.0, 4.0, (EXPERTS, D, FF))
    return entries * scales * D ** (-0.5)


def draw_w_gate(key, part):
    return column_scaled(key, 11).astype(jnp.bfloat16)


def draw_w_up(key, part):
    return column_scaled(key, 12).astype(jnp.bfloat16)


def block_levels(rng, shape, pieces, least, top_value):
    level = 1.0
    for dim, shards_of in pieces:
        draws = jax.random.uniform(jax.random.fold_in(jax.random.fold_in(rng, 6), dim), (shards_of,), jnp.float32, least / len(pieces), top_value / len(pieces))
        level = level * jnp.repeat(jnp.exp(draws), shape[dim] // shards_of).reshape((-1,) + (1,) * (len(shape) - 1 - dim))
    return level


def deal_out(rng, own, number, rows, number_of, top, limit, skew):
    sequence = jax.random.permutation(rng, number_of)
    crowded, ordinary = shares(number_of, rows * top, limit, skew, True), shares(number_of, rows * top, limit, skew, False)
    places = jnp.arange(number_of)

    def named(tallies, turn):
        used = int((tallies > 0).sum())
        fixed = max(1, used // 4)
        shifted = fixed + (places - fixed + turn * (used - fixed)) % max(1, number_of - fixed)
        return jnp.zeros((number_of,), jnp.int32).at[sequence[jnp.where(places < fixed, places, shifted)]].set(jnp.asarray(tallies, jnp.int32))

    tallies = jnp.where(number % 4 == 0, named(crowded, number // 4), named(ordinary, number - number // 4 - 1))
    mixed = jax.random.permutation(jax.random.fold_in(own, 3), number_of)
    source_of, receiver = mixed[0:number_of // 2 * 2:2], mixed[1:number_of // 2 * 2:2]
    margin = jnp.minimum(tallies[source_of] - 1, limit - tallies[receiver]) // 2
    margin = jnp.where((source_of == sequence[0]) | (receiver == sequence[0]) | (tallies[receiver] == 0), 0, jnp.maximum(margin, 0))
    shifted = jax.random.randint(jax.random.fold_in(own, 4), (number_of // 2,), 0, 1 << 20) % (margin + 1)
    tallies = tallies.at[source_of].add(-shifted).at[receiver].add(shifted)
    items = jnp.searchsorted(jnp.cumsum(tallies), jnp.arange(rows * top), side="right").astype(jnp.int32)
    listing = items.reshape(top, rows).T
    listing = listing[jax.random.permutation(jax.random.fold_in(own, 1), rows)]
    turn = jax.random.randint(jax.random.fold_in(own, 2), (rows, 1), 0, top)
    return jnp.take_along_axis(listing, (jnp.arange(top)[None, :] + turn) % top, axis=1)


def shares(amount, total, reach, skew, full):
    weights = [(1 << 20) // math.isqrt(rank ** skew) + 1 for rank in range(1, amount + 1)]
    largest = reach if full else min(reach, max(-(-total // amount), total * weights[0] // sum(weights)))
    least = 1 if total - largest >= amount - 1 else 0
    counts, surplus = [largest] + [least] * (amount - 1), total - largest - least * (amount - 1)
    while surplus > 0:
        free = [i for i in range(1, amount) if counts[i] < largest] or [i for i in range(1, amount) if counts[i] < reach]
        whole, left = sum([weights[i] for i in free]), surplus
        for i in free:
            more = min(reach - counts[i], max(1, left * weights[i] // whole), surplus)
            counts[i] = counts[i] + more
            surplus = surplus - more
    return np.array(counts)


def normal_values(rng, extent, scale, bound, cuts=(), held_as=jnp.bfloat16):
    values = scale * jax.random.normal(rng, extent, jnp.float32)
    if cuts:
        values = values * block_levels(rng, extent, cuts, -0.22, 0.18)
    return jnp.clip(values, -bound, bound).astype(held_as)


def setup_inputs(seed: int = 0) -> dict:
    arg_keys = jax.random.split(jax.random.key(seed), 15)
    residual_in = normal_values(arg_keys[0], (TOKEN_COUNT, D), 1.0, 6.0, ((0, 32),))
    queries = normal_values(arg_keys[1], (TOKEN_COUNT, HEADS * DK), 1.0, 6.0, ((0, 8), (1, 4)))
    key_rows = normal_values(arg_keys[2], (TOKEN_COUNT, HEADS * DK), 1.0, 6.0, ((0, 8), (1, 4)))
    value_rows = normal_values(arg_keys[3], (TOKEN_COUNT, HEADS * DV), 1.0, 6.0, ((0, 8), (1, 4)))
    out_gate = normal_values(arg_keys[4], (TOKEN_COUNT, HEADS * DV), 1.0, 6.0, ((0, 8), (1, 4)))
    decay_logit = draw_decay_logit(jax.random.fold_in(arg_keys[14], 71), 0)
    head_gain = jnp.clip(1.0 + 0.18 * jax.random.normal(arg_keys[6], (DV,), jnp.float32), 0.099609375, 1.8984375).astype(jnp.bfloat16)
    w_out = normal_values(arg_keys[7], (HEADS * DV, D), (HEADS * DV) ** -0.5, 0.1875)
    ffn_gain = jnp.clip(1.0 + 0.18 * jax.random.normal(arg_keys[8], (D,), jnp.float32), 0.099609375, 1.8984375).astype(jnp.bfloat16)
    routing_keys = jax.random.split(jax.random.fold_in(arg_keys[9], 1), TOKEN_COUNT // QROWS)
    routing_turns = jax.random.permutation(jax.random.fold_in(arg_keys[9], 3), TOKEN_COUNT // QROWS)
    routing = jax.vmap(lambda own, number: deal_out(jax.random.fold_in(arg_keys[9], 2), own, number, QROWS, EXPERTS, TOP, CAP, 2))(routing_keys, routing_turns).reshape((TOKEN_COUNT, TOP))
    route_weight = jnp.clip(jnp.exp(math.log(0.6) - 2.4849067 * jax.random.uniform(arg_keys[10], (TOKEN_COUNT, TOP), jnp.float32) ** block_levels(arg_keys[10], (TOKEN_COUNT, TOP), ((0, 32),), -0.2, 0.2)), 0.05, 0.6)
    w_gate = draw_w_gate(jax.random.fold_in(arg_keys[14], 71), 0)
    w_up = draw_w_up(jax.random.fold_in(arg_keys[14], 71), 0)
    w_down = normal_values(arg_keys[13], (EXPERTS, FF, D), FF ** -0.5, 0.125, ((0, 8), (1, 4)))
    return dict(residual_in=residual_in, queries=queries, key_rows=key_rows, value_rows=value_rows, out_gate=out_gate, decay_logit=decay_logit, head_gain=head_gain, w_out=w_out, ffn_gain=ffn_gain, routing=routing, route_weight=route_weight, w_gate=w_gate, w_up=w_up, w_down=w_down)


DECAY_TEMP = 16.0
CLAMP_LIMIT = 7.0
SIGMOID_SLOPE = 1.702
NORM_EPS = 1e-06
EXACT_PRECISION = lax.Precision.HIGHEST

def block_parts(query_blk, key_blk, value_blk, logdecay_blk):
    cumulative = jnp.cumsum(logdecay_blk, axis=2)
    length = cumulative.shape[2]
    causal = (jnp.arange(length)[:, None] >= jnp.arange(length)[None, :])[:, :, None]
    spread = cumulative[:, :, :, None, :] - cumulative[:, :, None, :, :]
    weighted = query_blk[:, :, :, None, :] * jnp.exp(jnp.where(causal, spread, -jnp.inf))
    scores = jnp.einsum('nhtsk,nhsk->nhts', weighted, key_blk, precision=EXACT_PRECISION)
    inner_part = jnp.einsum('nhts,nhsv->nhtv', scores, value_blk, precision=EXACT_PRECISION)
    ending = cumulative[:, :, -1:, :]
    contrib = jnp.einsum('nhsk,nhsv->nhkv', key_blk * jnp.exp(ending - cumulative), value_blk, precision=EXACT_PRECISION)
    return (inner_part, query_blk * jnp.exp(cumulative), contrib, jnp.exp(ending[:, :, 0, :]))

def carry_blocks(query_dec, contrib, passing, begin):

    def advance(recurrent_state, inputs):
        current_query, contrib_now, passing_now = inputs
        state_readout = jnp.einsum('uaz,uze->uae', current_query, recurrent_state, precision=EXACT_PRECISION)
        return (passing_now[..., None] * recurrent_state + contrib_now, state_readout)
    final_state, readouts = lax.scan(advance, begin, (query_dec, contrib, passing))
    return (readouts, final_state)

def finish_heads(blocks_out, head_gain, out_gate):
    count_blk, head_count, length, head_width = blocks_out.shape
    tokens = count_blk * length
    attended = blocks_out.transpose(0, 2, 1, 3).reshape(tokens, head_count, head_width)
    inv_scale = lax.rsqrt(lax.optimization_barrier(jnp.mean(attended * attended, axis=-1, keepdims=True)) + NORM_EPS)
    headed = attended * inv_scale * head_gain.astype(jnp.float32)
    gated = headed.reshape(tokens, head_count * head_width) * jax.nn.silu(out_gate.astype(jnp.float32))
    return gated.astype(jnp.bfloat16)

def norm_rows(residual, gain_vec):
    values = residual.astype(jnp.float32)
    inv_scale = lax.rsqrt(lax.optimization_barrier(jnp.mean(values * values, axis=-1, keepdims=True)) + NORM_EPS)
    return (values * inv_scale * gain_vec.astype(jnp.float32)).astype(jnp.bfloat16)

def clamped_unit(gate_pre, up_pre):
    gate_cut = jnp.minimum(gate_pre, CLAMP_LIMIT)
    up_cut = jnp.clip(up_pre, -CLAMP_LIMIT, CLAMP_LIMIT)
    return (up_cut + 1.0) * (gate_cut * jax.nn.sigmoid(SIGMOID_SLOPE * gate_cut))

def slot_ids(routes, capacity, experts):
    batch_size, rows_each, top_count = routes.shape
    flat_ids = routes.reshape(batch_size, rows_each * top_count)
    onehot = (flat_ids[:, :, None] == jnp.arange(experts, dtype=jnp.int32)[None, None, :]).astype(jnp.int32)
    earlier = jnp.cumsum(onehot, axis=1) - onehot
    rank_in = lax.optimization_barrier(jnp.sum(earlier * onehot, axis=2))
    return (flat_ids * capacity + rank_in).reshape(batch_size, rows_each, top_count)

def reference(residual_in, queries, key_rows, value_rows, out_gate, decay_logit, head_gain, w_out, ffn_gain, routing, route_weight, w_gate, w_up, w_down):
    groups = TOKEN_COUNT // TOK_DEV

    def grouped(array, head_width):
        shaped = array.astype(jnp.float32).reshape(groups, TOK_DEV // BLOCK, BLOCK, HEADS, head_width)
        return shaped.transpose(0, 1, 3, 2, 4)
    query_grp = grouped(queries, DK) * DK ** (-0.5)
    key_grp = grouped(key_rows, DK)
    value_grp = grouped(value_rows, DV)
    logdecay_grp = grouped(jax.nn.log_sigmoid(decay_logit) / DECAY_TEMP, DK)

    def through(recurrent_state, inputs):
        current_query, key_now, value_now, decay_now = inputs
        inner_part, query_dec, contrib, passing = block_parts(current_query, key_now, value_now, decay_now)
        readouts, final_state = carry_blocks(query_dec, contrib, passing, recurrent_state)
        return (final_state, inner_part + readouts)
    _, outputs = lax.scan(through, jnp.zeros((HEADS, DK, DV), jnp.float32), (query_grp, key_grp, value_grp, logdecay_grp))
    mixed_out = finish_heads(outputs.reshape(TOKEN_COUNT // BLOCK, HEADS, BLOCK, DV), head_gain, out_gate)
    projected = jnp.dot(mixed_out, w_out, preferred_element_type=jnp.float32)
    residual = (residual_in.astype(jnp.float32) + projected).astype(jnp.bfloat16)
    normed = norm_rows(residual, ffn_gain)
    blocks = TOKEN_COUNT // QROWS
    ranked = slot_ids(routing.reshape(blocks, QROWS, TOP), CAP, EXPERTS).reshape(blocks, QROWS * TOP)
    flat_expert = routing.reshape(blocks, QROWS * TOP)
    rank_in = ranked - flat_expert * CAP
    placed = (flat_expert * (blocks * CAP) + jnp.arange(blocks, dtype=jnp.int32)[:, None] * CAP + rank_in).reshape(-1)
    token_of = jnp.repeat(jnp.arange(TOKEN_COUNT, dtype=jnp.int32), TOP)
    slots_all = EXPERTS * blocks * CAP
    token_table = jnp.zeros((slots_all,), jnp.int32).at[placed].set(token_of).reshape(EXPERTS, blocks * CAP)
    weight_table = jnp.zeros((slots_all,), jnp.float32).at[placed].set(route_weight.reshape(-1)).reshape(EXPERTS, blocks * CAP)
    live_slot = jnp.zeros((slots_all,), jnp.float32).at[placed].set(1.0).reshape(EXPERTS, blocks * CAP)
    part_width = FF // N_TP

    def serve_expert(accumulated, inputs):
        token_ids, slot_weight, slot_live, gate_cols, up_cols, down_rows = inputs
        gathered = jnp.where(slot_live[:, None] > 0, normed[token_ids], jnp.zeros((), jnp.bfloat16))
        gate_pre = jnp.dot(gathered, gate_cols, preferred_element_type=jnp.float32)
        up_pre = jnp.dot(gathered, up_cols, preferred_element_type=jnp.float32)
        hidden = clamped_unit(gate_pre, up_pre).astype(jnp.bfloat16)
        expert_out = jnp.zeros((gathered.shape[0], D), jnp.float32)
        for shard_no in range(N_TP):
            portion = jnp.dot(hidden[:, shard_no * part_width:(shard_no + 1) * part_width], down_rows[shard_no * part_width:(shard_no + 1) * part_width], preferred_element_type=jnp.float32).astype(jnp.bfloat16)
            portion = lax.optimization_barrier(portion)
            expert_out = expert_out + portion.astype(jnp.float32)
        expert_out = expert_out.astype(jnp.bfloat16)
        return (accumulated.at[token_ids].add(slot_weight[:, None] * expert_out.astype(jnp.float32)), None)
    routed, _ = lax.scan(serve_expert, jnp.zeros((TOKEN_COUNT, D), jnp.float32), (token_table, weight_table, live_slot, w_gate, w_up, w_down))
    return (residual.astype(jnp.float32) + routed).astype(jnp.bfloat16)
```

```python
import jax
import jax.numpy as jnp
from jax import lax
from jax.experimental import pallas as pl
from jax.experimental.pallas import tpu as pltpu
from jax.sharding import PartitionSpec as P
import functools

DK = 64
DV = 128


DECAY_TEMP = 16.0
CLAMP_LIMIT = 7.0
SIGMOID_SLOPE = 1.702
NORM_EPS = 1e-06
EXACT_PRECISION = lax.Precision.HIGHEST


def clamped_unit(gate_pre, up_pre):
    gate_cut = jnp.minimum(gate_pre, CLAMP_LIMIT)
    up_cut = jnp.clip(up_pre, -CLAMP_LIMIT, CLAMP_LIMIT)
    return (up_cut + 1.0) * (gate_cut * jax.nn.sigmoid(SIGMOID_SLOPE * gate_cut))


MESH = pl.DeviceIdType.MESH
LANES = 128
SUB = 32
EXP_CAP = 64.0


def nt_dot(left, right):
    return lax.dot_general(
        left, right, (((1,), (1,)), ((), ())), preferred_element_type=jnp.float32
    )


def tn_dot(left, right):
    return lax.dot_general(
        left, right, (((0,), (0,)), ((), ())), preferred_element_type=jnp.float32
    )


def mix_kernel(
    sp_count, tp_count,
    q_ref, k_ref, v_ref, gate_ref, decay_ref, head_gain_ref, w_hbm, ffn_gain_ref,
    routing_ref, weight_ref, res_in_ref,
    res_ref, ext_ref,
    states, attended, mixed, mixed_in, w_vmem,
    w_sem, state_send, state_recv, mix_send, mix_recv,
):
    sp_me, tp_me = lax.axis_index("sp"), lax.axis_index("tp")
    barrier = pltpu.get_barrier_semaphore()

    @pl.loop(1, sp_count)
    def _(d):
        pl.semaphore_signal(
            barrier, inc=1, device_id={"sp": lax.rem(sp_me + d, sp_count)}, device_id_type=MESH
        )

    @pl.loop(1, tp_count)
    def _(d):
        pl.semaphore_signal(
            barrier, inc=1, device_id={"tp": lax.rem(tp_me + d, tp_count)}, device_id_type=MESH
        )

    w_copy = pltpu.make_async_copy(w_hbm, w_vmem, w_sem)
    w_copy.start()

    tokens, key_lanes = q_ref.shape
    value_lanes = v_ref.shape[1]
    head_count = key_lanes // DK
    lane_head = lax.broadcasted_iota(jnp.int32, (1, key_lanes), 1) // DK
    logit = decay_ref[...]
    log_decay = (jnp.minimum(logit, 0.0) - jnp.log1p(jnp.exp(-jnp.abs(logit)))) / DECAY_TEMP
    row_id = lax.broadcasted_iota(jnp.int32, (tokens, tokens), 0)
    col_id = lax.broadcasted_iota(jnp.int32, (tokens, tokens), 1)
    lower = (row_id >= col_id).astype(jnp.float32)
    cumulative = jnp.dot(
        lower, log_decay, precision=EXACT_PRECISION, preferred_element_type=jnp.float32
    )
    keys = k_ref[...].astype(jnp.float32)
    query = q_ref[...].astype(jnp.float32) * DK ** (-0.5)
    values = v_ref[...]
    ending = cumulative[tokens - 1 :, :]
    wide = tn_dot(values, (keys * jnp.exp(ending - cumulative)).astype(jnp.bfloat16))
    state = jnp.zeros((DV, key_lanes), jnp.float32)
    for h in range(head_count):
        state = jnp.where(lane_head == h, wide[h * DV : (h + 1) * DV, :], state)
    passing = jnp.exp(ending)
    passing_hi = passing.astype(jnp.bfloat16).astype(jnp.float32)
    tail_row = lax.broadcasted_iota(jnp.int32, (16, key_lanes), 0)
    tail = jnp.where(
        tail_row == 0, passing_hi, jnp.where(tail_row == 1, passing - passing_hi, 0.0)
    )
    states[sp_me, 0:DV, :] = state.astype(jnp.bfloat16)
    states[sp_me, DV : DV + 16, :] = tail.astype(jnp.bfloat16)

    pl.semaphore_wait(barrier, sp_count + tp_count - 2)

    def state_copy(slot, d):
        return pltpu.make_async_remote_copy(
            src_ref=states.at[slot],
            dst_ref=states.at[slot],
            send_sem=state_send.at[d],
            recv_sem=state_recv.at[slot],
            device_id={"sp": lax.rem(sp_me + d, sp_count)},
            device_id_type=MESH,
        )

    @pl.loop(1, sp_count)
    def _(d):
        state_copy(sp_me, d).start()

    for i in range(tokens // SUB):
        first = i * SUB
        reach = min(-(-(first + SUB) // LANES) * LANES, tokens)
        start = cumulative[first - 1 : first, :] if i else jnp.zeros((1, key_lanes), jnp.float32)
        q_sub = query[first : first + SUB] * jnp.exp(cumulative[first : first + SUB] - start)
        k_sub = keys[:reach] * jnp.exp(jnp.minimum(start - cumulative[:reach], EXP_CAP))
        stacked = jnp.concatenate(
            [jnp.where(lane_head == h, q_sub, 0.0) for h in range(head_count)], axis=0
        )
        scores = nt_dot(stacked.astype(jnp.bfloat16), k_sub.astype(jnp.bfloat16))
        at_row = lax.broadcasted_iota(jnp.int32, scores.shape, 0) % SUB + first
        at_col = lax.broadcasted_iota(jnp.int32, scores.shape, 1)
        scores = jnp.where(at_row >= at_col, scores, 0.0).astype(jnp.bfloat16)
        inner = jnp.dot(scores, values[:reach], preferred_element_type=jnp.float32)
        for h in range(head_count):
            attended[first : first + SUB, h * DV : (h + 1) * DV] = inner[
                h * SUB : (h + 1) * SUB, h * DV : (h + 1) * DV
            ]

    @pl.loop(1, sp_count)
    def _(d):
        state_copy(lax.rem(sp_me + d, sp_count), d).wait_recv()

    def absorb(j, incoming):
        decay = states[j, DV : DV + 16, :].astype(jnp.float32)
        total = decay[0:1, :] + decay[1:2, :]
        following = total * incoming + states[j, 0:DV, :].astype(jnp.float32)
        return jnp.where(j < sp_me, following, incoming)

    incoming = lax.fori_loop(
        0, sp_count, absorb, jnp.zeros((DV, key_lanes), jnp.float32)
    ).astype(jnp.bfloat16)
    query_dec = query * jnp.exp(cumulative)
    for h in range(head_count):
        cols = slice(h * DV, (h + 1) * DV)
        readout = nt_dot(jnp.where(lane_head == h, query_dec, 0.0).astype(jnp.bfloat16), incoming)
        head = attended[:, cols] + readout
        scale = lax.rsqrt(jnp.mean(head * head, axis=-1, keepdims=True) + NORM_EPS)
        opened = gate_ref[:, cols].astype(jnp.float32)
        opened = opened * jax.nn.sigmoid(opened)
        mixed[:, cols] = (head * scale * head_gain_ref[...].astype(jnp.float32) * opened).astype(
            jnp.bfloat16
        )

    rows = res_in_ref.shape[0]

    def mix_copy(block, slot, d):
        return pltpu.make_async_remote_copy(
            src_ref=mixed.at[pl.ds(pl.multiple_of(block * rows, rows), rows)],
            dst_ref=mixed_in.at[slot],
            send_sem=mix_send.at[d],
            recv_sem=mix_recv.at[slot],
            device_id={"tp": lax.rem(tp_me + d, tp_count)},
            device_id_type=MESH,
        )

    for d in range(1, tp_count):
        mix_copy(lax.rem(tp_me + d, tp_count), tp_me, d).start()

    lane = lax.broadcasted_iota(jnp.int32, (rows, LANES), 1)
    named = routing_ref[pl.ds(pl.multiple_of(tp_me * rows, rows), rows), :]
    share = jnp.zeros((rows, LANES), jnp.float32)
    for j in range(weight_ref.shape[1]):
        share = share + jnp.where(
            lane % (LANES // 2) == named[:, j : j + 1], weight_ref[:, j : j + 1], 0.0
        )
    share_hi = share.astype(jnp.bfloat16).astype(jnp.float32)
    width = res_in_ref.shape[1]
    ext_ref[:, width:] = jnp.where(lane < LANES // 2, share_hi, share - share_hi).astype(
        jnp.bfloat16
    )

    w_copy.wait()

    def w_rows(j):
        return w_vmem[pl.ds(pl.multiple_of(j * value_lanes, value_lanes), value_lanes), :]

    projected = jnp.dot(
        mixed[pl.ds(pl.multiple_of(tp_me * rows, rows), rows), :],
        w_rows(tp_me),
        preferred_element_type=jnp.float32,
    )
    for d in range(1, tp_count):
        slot = lax.rem(tp_me + d, tp_count)
        mix_copy(slot, slot, d).wait_recv()
        projected = projected + jnp.dot(
            mixed_in[slot], w_rows(slot), preferred_element_type=jnp.float32
        )
    residual = (res_in_ref[...].astype(jnp.float32) + projected).astype(jnp.bfloat16)
    res_ref[...] = residual
    wide_res = residual.astype(jnp.float32)
    inv = lax.rsqrt(jnp.mean(wide_res * wide_res, axis=-1, keepdims=True) + NORM_EPS)
    ext_ref[:, :width] = (wide_res * inv * ffn_gain_ref[...].astype(jnp.float32)).astype(
        jnp.bfloat16
    )

    @pl.loop(1, sp_count)
    def _(d):
        state_copy(sp_me, d).wait_send()

    for d in range(1, tp_count):
        mix_copy(lax.rem(tp_me + d, tp_count), tp_me, d).wait_send()


def mix_rows(
    queries, key_rows, value_rows, out_gate, decay_logit, head_gain, w_out,
    ffn_gain, routing, route_weight, residual_in,
):
    sp_count, tp_count = lax.axis_size("sp"), lax.axis_size("tp")
    rows, width = residual_in.shape
    tokens, key_lanes = queries.shape
    value_lanes = value_rows.shape[1]
    vmem = pl.BlockSpec(memory_space=pltpu.VMEM)
    return pl.pallas_call(
        functools.partial(mix_kernel, sp_count, tp_count),
        out_shape=(
            jax.ShapeDtypeStruct((rows, width), jnp.bfloat16),
            jax.ShapeDtypeStruct((rows, width + LANES), jnp.bfloat16),
        ),
        in_specs=[vmem] * 6 + [pl.BlockSpec(memory_space=pl.ANY)] + [vmem] * 4,
        out_specs=(vmem, vmem),
        scratch_shapes=[
            pltpu.VMEM((sp_count, DV + 16, key_lanes), jnp.bfloat16),
            pltpu.VMEM((tokens, value_lanes), jnp.float32),
            pltpu.VMEM((tokens, value_lanes), jnp.bfloat16),
            pltpu.VMEM((tp_count, rows, value_lanes), jnp.bfloat16),
            pltpu.VMEM(w_out.shape, jnp.bfloat16),
            pltpu.SemaphoreType.DMA,
            pltpu.SemaphoreType.DMA((sp_count,)),
            pltpu.SemaphoreType.DMA((sp_count,)),
            pltpu.SemaphoreType.DMA((tp_count,)),
            pltpu.SemaphoreType.DMA((tp_count,)),
        ],
        compiler_params=pltpu.CompilerParams(
            collective_id=0, has_side_effects=True, vmem_limit_bytes=40 << 20
        ),
        name="mix_rows",
    )(
        queries, key_rows, value_rows, out_gate, decay_logit, head_gain.reshape(1, -1), w_out,
        ffn_gain.reshape(1, -1), routing, route_weight, residual_in,
    )


def expert_kernel(x_ref, share_ref, gate_ref, up_ref, down_ref, out_ref):
    rows = x_ref[...]
    gate_pre = jnp.dot(rows, gate_ref[...], preferred_element_type=jnp.float32)
    up_pre = jnp.dot(rows, up_ref[...], preferred_element_type=jnp.float32)
    hidden = clamped_unit(gate_pre, up_pre).astype(jnp.bfloat16)
    lane = lax.broadcasted_iota(jnp.int32, share_ref.shape, 1) % (LANES // 2)
    share = jnp.sum(
        jnp.where(lane == lax.axis_index("sp"), share_ref[...].astype(jnp.float32), 0.0),
        axis=-1,
        keepdims=True,
    )
    out = jnp.dot(hidden, down_ref[...], preferred_element_type=jnp.float32)
    out_ref[...] = (out * share).astype(jnp.bfloat16)


def expert_rows(everyone, gate_cols, up_cols, down_rows):
    tokens = everyone.shape[0]
    width, units = gate_cols.shape
    step = min(256, tokens)
    return pl.pallas_call(
        expert_kernel,
        grid=(tokens // step,),
        out_shape=jax.ShapeDtypeStruct((tokens, width), jnp.bfloat16),
        in_specs=[
            pl.BlockSpec((step, width), lambda i: (i, 0)),
            pl.BlockSpec((step, LANES), lambda i: (i, width // LANES)),
            pl.BlockSpec((width, units), lambda i: (0, 0)),
            pl.BlockSpec((width, units), lambda i: (0, 0)),
            pl.BlockSpec((units, width), lambda i: (0, 0)),
        ],
        out_specs=pl.BlockSpec((step, width), lambda i: (i, 0)),
        compiler_params=pltpu.CompilerParams(vmem_limit_bytes=48 << 20),
        cost_estimate=pl.CostEstimate(
            flops=6 * tokens * width * units, bytes_accessed=8 * tokens * width, transcendentals=0
        ),
        name="expert_rows",
    )(everyone, everyone, gate_cols, up_cols, down_rows)


def slot_ids(routes, capacity, experts):
    batch_size, rows_each, top_count = routes.shape
    flat_ids = routes.reshape(batch_size, rows_each * top_count)
    onehot = (flat_ids[:, :, None] == jnp.arange(experts, dtype=jnp.int32)[None, None, :]).astype(
        jnp.int32
    )
    earlier = jnp.cumsum(onehot, axis=1) - onehot
    rank_in = jnp.sum(earlier * onehot, axis=2)
    return (flat_ids * capacity + rank_in).reshape(batch_size, rows_each, top_count)


def dispatch_rows(slots, row_data, slot_total):
    chosen = jnp.any(slots[..., None] == jnp.arange(slot_total, dtype=jnp.int32), axis=2).astype(
        jnp.bfloat16
    )
    return jnp.einsum("brs,brd->bsd", chosen, row_data, preferred_element_type=jnp.float32).astype(
        jnp.bfloat16
    )


def on_device(
    residual_in,
    queries,
    key_rows,
    value_rows,
    out_gate,
    decay_logit,
    head_gain,
    w_out,
    ffn_gain,
    routing,
    route_weight,
    w_gate,
    w_up,
    w_down,
):
    tp_count = lax.axis_size("tp")
    experts = lax.axis_size("sp")
    quarter = residual_in.shape[0]
    top_count = routing.shape[1]
    model_width = residual_in.shape[1]
    capacity = 2 * routing.shape[0] * top_count // (tp_count * experts)
    slot_total = experts * capacity
    residual, extended = mix_rows(
        queries, key_rows, value_rows, out_gate, decay_logit, head_gain, w_out,
        ffn_gain, routing, route_weight, residual_in,
    )
    if capacity >= quarter and experts <= LANES // 2:
        everyone = lax.all_gather(extended, ("sp", "tp"), axis=0, tiled=True)
        partial_rows = expert_rows(everyone, w_gate[0], w_up[0], w_down[0])
        routed = lax.psum_scatter(
            partial_rows, ("sp", "tp"), scatter_dimension=0, tiled=True
        ).astype(jnp.float32)
        return (residual.astype(jnp.float32) + routed).astype(jnp.bfloat16)
    normed = extended[:, :model_width]
    gate_cols = w_gate[0]
    up_cols = w_up[0]
    down_rows = w_down[0]
    own_routes = lax.dynamic_slice_in_dim(routing, lax.axis_index("tp") * quarter, quarter, 0)
    own_slots = slot_ids(own_routes[None], capacity, experts)[0]
    outgoing = dispatch_rows(own_slots[None], normed[None], slot_total)[0]
    arrived = lax.all_to_all(
        outgoing.reshape(experts, capacity, model_width),
        "sp",
        split_axis=0,
        concat_axis=0,
        tiled=True,
    )
    portion = lax.all_gather(arrived[None], "tp", axis=0, tiled=True)
    flat_rows = portion.reshape(-1, model_width)
    gate_pre = jnp.dot(flat_rows, gate_cols, preferred_element_type=jnp.float32)
    up_pre = jnp.dot(flat_rows, up_cols, preferred_element_type=jnp.float32)
    hidden_rows = clamped_unit(gate_pre, up_pre).astype(jnp.bfloat16)
    hidden = hidden_rows.reshape(portion.shape[:-1] + (gate_cols.shape[1],))
    portion = hidden
    partial_out = jnp.dot(
        portion.reshape(-1, hidden.shape[-1]), down_rows, preferred_element_type=jnp.float32
    ).astype(jnp.bfloat16)
    partial_out = lax.optimization_barrier(partial_out)
    summed = lax.psum_scatter(
        partial_out.astype(jnp.float32)
        .reshape(portion.shape[:-1] + (model_width,))
        .astype(jnp.bfloat16),
        "tp",
        scatter_dimension=0,
        tiled=True,
    ).astype(jnp.float32)
    returned = lax.all_to_all(
        summed[0].astype(jnp.bfloat16), "sp", split_axis=0, concat_axis=0, tiled=True
    )
    picked = jnp.take(
        returned.reshape(slot_total, model_width), own_slots.reshape(-1), axis=0
    ).reshape(quarter, top_count, model_width)
    routed = jnp.sum(picked.astype(jnp.float32) * route_weight[:, :, None], axis=1)
    return (residual.astype(jnp.float32) + routed).astype(jnp.bfloat16)


def solution(mesh):
    placed = (
        P(("sp", "tp"), None),
        P("sp", "tp"),
        P("sp", "tp"),
        P("sp", "tp"),
        P("sp", "tp"),
        P("sp", "tp"),
        P(),
        P(),
        P(),
        P("sp", None),
        P(("sp", "tp"), None),
        P("sp", None, "tp"),
        P("sp", None, "tp"),
        P("sp", "tp", None),
    )
    return jax.shard_map(
        on_device, mesh=mesh, in_specs=placed, out_specs=P(("sp", "tp"), None), check_vma=False
    )
```

```python
import jax
import jax.numpy as jnp
from jax import lax
from jax.experimental import pallas as pl
from jax.experimental.pallas import tpu as pltpu
from jax.sharding import PartitionSpec as P
import functools

DK = 64
DV = 128


DECAY_TEMP = 16.0
CLAMP_LIMIT = 7.0
SIGMOID_SLOPE = 1.702
NORM_EPS = 1e-06
EXACT_PRECISION = lax.Precision.HIGHEST


def clamped_unit(gate_pre, up_pre):
    gate_cut = jnp.minimum(gate_pre, CLAMP_LIMIT)
    up_cut = jnp.clip(up_pre, -CLAMP_LIMIT, CLAMP_LIMIT)
    return (up_cut + 1.0) * (gate_cut * jax.nn.sigmoid(SIGMOID_SLOPE * gate_cut))


MESH = pl.DeviceIdType.MESH
LANES = 128
SUB = 32
EXP_CAP = 64.0


def nt_dot(left, right):
    return lax.dot_general(
        left, right, (((1,), (1,)), ((), ())), preferred_element_type=jnp.float32
    )


def tn_dot(left, right):
    return lax.dot_general(
        left, right, (((0,), (0,)), ((), ())), preferred_element_type=jnp.float32
    )


def mix_kernel(
    sp_count, tp_count,
    q_ref, k_ref, v_ref, gate_ref, decay_ref, head_gain_ref, w_hbm, ffn_gain_ref,
    routing_ref, weight_ref, res_in_ref,
    res_ref, ext_ref,
    states, attended, mixed, mixed_in, w_vmem,
    w_sem, state_send, state_recv, mix_send, mix_recv,
):
    sp_me, tp_me = lax.axis_index("sp"), lax.axis_index("tp")
    barrier = pltpu.get_barrier_semaphore()

    @pl.loop(1, sp_count)
    def _(d):
        pl.semaphore_signal(
            barrier, inc=1, device_id={"sp": lax.rem(sp_me + d, sp_count)}, device_id_type=MESH
        )

    @pl.loop(1, tp_count)
    def _(d):
        pl.semaphore_signal(
            barrier, inc=1, device_id={"tp": lax.rem(tp_me + d, tp_count)}, device_id_type=MESH
        )

    w_copy = pltpu.make_async_copy(w_hbm, w_vmem, w_sem)
    w_copy.start()

    tokens, key_lanes = q_ref.shape
    value_lanes = v_ref.shape[1]
    head_count = key_lanes // DK
    lane_head = lax.broadcasted_iota(jnp.int32, (1, key_lanes), 1) // DK
    logit = decay_ref[...]
    log_decay = (jnp.minimum(logit, 0.0) - jnp.log1p(jnp.exp(-jnp.abs(logit)))) / DECAY_TEMP
    row_id = lax.broadcasted_iota(jnp.int32, (tokens, tokens), 0)
    col_id = lax.broadcasted_iota(jnp.int32, (tokens, tokens), 1)
    lower = (row_id >= col_id).astype(jnp.float32)
    cumulative = jnp.dot(
        lower, log_decay, precision=EXACT_PRECISION, preferred_element_type=jnp.float32
    )
    keys = k_ref[...].astype(jnp.float32)
    query = q_ref[...].astype(jnp.float32) * DK ** (-0.5)
    values = v_ref[...]
    ending = cumulative[tokens - 1 :, :]
    wide = tn_dot(values, (keys * jnp.exp(ending - cumulative)).astype(jnp.bfloat16))
    state = jnp.zeros((DV, key_lanes), jnp.float32)
    for h in range(head_count):
        state = jnp.where(lane_head == h, wide[h * DV : (h + 1) * DV, :], state)
    passing = jnp.exp(ending)
    passing_hi = passing.astype(jnp.bfloat16).astype(jnp.float32)
    tail_row = lax.broadcasted_iota(jnp.int32, (16, key_lanes), 0)
    tail = jnp.where(
        tail_row == 0, passing_hi, jnp.where(tail_row == 1, passing - passing_hi, 0.0)
    )
    states[sp_me, 0:DV, :] = state.astype(jnp.bfloat16)
    states[sp_me, DV : DV + 16, :] = tail.astype(jnp.bfloat16)

    pl.semaphore_wait(barrier, sp_count + tp_count - 2)

    def state_copy(slot, d):
        return pltpu.make_async_remote_copy(
            src_ref=states.at[slot],
            dst_ref=states.at[slot],
            send_sem=state_send.at[d],
            recv_sem=state_recv.at[slot],
            device_id={"sp": lax.rem(sp_me + d, sp_count)},
            device_id_type=MESH,
        )

    @pl.loop(1, sp_count)
    def _(d):
        state_copy(sp_me, d).start()

    for i in range(tokens // SUB):
        first = i * SUB
        reach = min(-(-(first + SUB) // LANES) * LANES, tokens)
        start = cumulative[first - 1 : first, :] if i else jnp.zeros((1, key_lanes), jnp.float32)
        q_sub = query[first : first + SUB] * jnp.exp(cumulative[first : first + SUB] - start)
        k_sub = keys[:reach] * jnp.exp(jnp.minimum(start - cumulative[:reach], EXP_CAP))
        stacked = jnp.concatenate(
            [jnp.where(lane_head == h, q_sub, 0.0) for h in range(head_count)], axis=0
        )
        scores = nt_dot(stacked.astype(jnp.bfloat16), k_sub.astype(jnp.bfloat16))
        at_row = lax.broadcasted_iota(jnp.int32, scores.shape, 0) % SUB + first
        at_col = lax.broadcasted_iota(jnp.int32, scores.shape, 1)
        scores = jnp.where(at_row >= at_col, scores, 0.0).astype(jnp.bfloat16)
        inner = jnp.dot(scores, values[:reach], preferred_element_type=jnp.float32)
        for h in range(head_count):
            attended[first : first + SUB, h * DV : (h + 1) * DV] = inner[
                h * SUB : (h + 1) * SUB, h * DV : (h + 1) * DV
            ]

    @pl.loop(1, sp_count)
    def _(d):
        state_copy(lax.rem(sp_me + d, sp_count), d).wait_recv()

    def absorb(j, incoming):
        decay = states[j, DV : DV + 16, :].astype(jnp.float32)
        total = decay[0:1, :] + decay[1:2, :]
        following = total * incoming + states[j, 0:DV, :].astype(jnp.float32)
        return jnp.where(j < sp_me, following, incoming)

    incoming = lax.fori_loop(
        0, sp_count, absorb, jnp.zeros((DV, key_lanes), jnp.float32)
    ).astype(jnp.bfloat16)
    query_dec = query * jnp.exp(cumulative)
    for h in range(head_count):
        cols = slice(h * DV, (h + 1) * DV)
        readout = nt_dot(jnp.where(lane_head == h, query_dec, 0.0).astype(jnp.bfloat16), incoming)
        head = attended[:, cols] + readout
        scale = lax.rsqrt(jnp.mean(head * head, axis=-1, keepdims=True) + NORM_EPS)
        opened = gate_ref[:, cols].astype(jnp.float32)
        opened = opened * jax.nn.sigmoid(opened)
        mixed[:, cols] = (head * scale * head_gain_ref[...].astype(jnp.float32) * opened).astype(
            jnp.bfloat16
        )

    rows = res_in_ref.shape[0]

    def mix_copy(block, slot, d):
        return pltpu.make_async_remote_copy(
            src_ref=mixed.at[pl.ds(pl.multiple_of(block * rows, rows), rows)],
            dst_ref=mixed_in.at[slot],
            send_sem=mix_send.at[d],
            recv_sem=mix_recv.at[slot],
            device_id={"tp": lax.rem(tp_me + d, tp_count)},
            device_id_type=MESH,
        )

    for d in range(1, tp_count):
        mix_copy(lax.rem(tp_me + d, tp_count), tp_me, d).start()

    lane = lax.broadcasted_iota(jnp.int32, (rows, LANES), 1)
    named = routing_ref[pl.ds(pl.multiple_of(tp_me * rows, rows), rows), :]
    share = jnp.zeros((rows, LANES), jnp.float32)
    for j in range(weight_ref.shape[1]):
        share = share + jnp.where(
            lane % (LANES // 2) == named[:, j : j + 1], weight_ref[:, j : j + 1], 0.0
        )
    share_hi = share.astype(jnp.bfloat16).astype(jnp.float32)
    width = res_in_ref.shape[1]
    ext_ref[:, width:] = jnp.where(lane < LANES // 2, share_hi, share - share_hi).astype(
        jnp.bfloat16
    )

    w_copy.wait()

    def w_rows(j):
        return w_vmem[pl.ds(pl.multiple_of(j * value_lanes, value_lanes), value_lanes), :]

    projected = jnp.dot(
        mixed[pl.ds(pl.multiple_of(tp_me * rows, rows), rows), :],
        w_rows(tp_me),
        preferred_element_type=jnp.float32,
    )
    for d in range(1, tp_count):
        slot = lax.rem(tp_me + d, tp_count)
        mix_copy(slot, slot, d).wait_recv()
        projected = projected + jnp.dot(
            mixed_in[slot], w_rows(slot), preferred_element_type=jnp.float32
        )
    residual = (res_in_ref[...].astype(jnp.float32) + projected).astype(jnp.bfloat16)
    res_ref[...] = residual
    wide_res = residual.astype(jnp.float32)
    inv = lax.rsqrt(jnp.mean(wide_res * wide_res, axis=-1, keepdims=True) + NORM_EPS)
    ext_ref[:, :width] = (wide_res * inv * ffn_gain_ref[...].astype(jnp.float32)).astype(
        jnp.bfloat16
    )

    @pl.loop(1, sp_count)
    def _(d):
        state_copy(sp_me, d).wait_send()

    for d in range(1, tp_count):
        mix_copy(lax.rem(tp_me + d, tp_count), tp_me, d).wait_send()


def mix_rows(
    queries, key_rows, value_rows, out_gate, decay_logit, head_gain, w_out,
    ffn_gain, routing, route_weight, residual_in,
):
    sp_count, tp_count = lax.axis_size("sp"), lax.axis_size("tp")
    rows, width = residual_in.shape
    tokens, key_lanes = queries.shape
    value_lanes = value_rows.shape[1]
    vmem = pl.BlockSpec(memory_space=pltpu.VMEM)
    return pl.pallas_call(
        functools.partial(mix_kernel, sp_count, tp_count),
        out_shape=(
            jax.ShapeDtypeStruct((rows, width), jnp.bfloat16),
            jax.ShapeDtypeStruct((rows, width + LANES), jnp.bfloat16),
        ),
        in_specs=[vmem] * 6 + [pl.BlockSpec(memory_space=pl.ANY)] + [vmem] * 4,
        out_specs=(vmem, vmem),
        scratch_shapes=[
            pltpu.VMEM((sp_count, DV + 16, key_lanes), jnp.bfloat16),
            pltpu.VMEM((tokens, value_lanes), jnp.float32),
            pltpu.VMEM((tokens, value_lanes), jnp.bfloat16),
            pltpu.VMEM((tp_count, rows, value_lanes), jnp.bfloat16),
            pltpu.VMEM(w_out.shape, jnp.bfloat16),
            pltpu.SemaphoreType.DMA,
            pltpu.SemaphoreType.DMA((sp_count,)),
            pltpu.SemaphoreType.DMA((sp_count,)),
            pltpu.SemaphoreType.DMA((tp_count,)),
            pltpu.SemaphoreType.DMA((tp_count,)),
        ],
        compiler_params=pltpu.CompilerParams(
            collective_id=0, has_side_effects=True, vmem_limit_bytes=40 << 20
        ),
        name="mix_rows",
    )(
        queries, key_rows, value_rows, out_gate, decay_logit, head_gain.reshape(1, -1), w_out,
        ffn_gain.reshape(1, -1), routing, route_weight, residual_in,
    )


def expert_kernel(
    z_count, y_count, gather_cuts, reduce_cuts,
    ext_ref, res_ref, gate_hbm, up_hbm, down_hbm, out_ref,
    rows_all, gate_w, up_w, down_w, hidden, shares, parts, got_core, got_first, got_second, got_z,
    w_sem, own_sem, gather_send, gather_recv, reduce_send, reduce_recv,
):
    sp_me, tp_me = lax.axis_index("sp"), lax.axis_index("tp")
    z, x = sp_me // 2, lax.rem(sp_me, 2)
    y, c = tp_me // 2, lax.rem(tp_me, 2)
    partner = {
        "x": {"sp": z * 2 + 1 - x},
        "y": {"tp": (1 - y) * 2 + c},
        "c": {"tp": y * 2 + 1 - c},
    }
    barrier = pltpu.get_barrier_semaphore()

    def z_peer(d):
        return {"sp": lax.rem(z + d, z_count) * 2 + x}

    for target in [z_peer(d) for d in range(1, z_count)] + list(partner.values()):
        pl.semaphore_signal(barrier, inc=1, device_id=target, device_id_type=MESH)
    loads = [
        pltpu.make_async_copy(src, dst, w_sem.at[i])
        for i, (src, dst) in enumerate(((gate_hbm, gate_w), (up_hbm, up_w), (down_hbm, down_w)))
    ]
    own = pltpu.make_async_copy(ext_ref, rows_all.at[z, x, y, c], own_sem)
    own.start()
    for load in loads:
        load.start()
    own.wait()
    pl.semaphore_wait(barrier, z_count + 2)

    def remote(src, dst, send, recv, target):
        return pltpu.make_async_remote_copy(
            src_ref=src, dst_ref=dst, send_sem=send, recv_sem=recv,
            device_id=target, device_id_type=MESH,
        )

    def gather_copies(i, stage, arriving):
        cols = pl.ds(gather_cuts[i][0], gather_cuts[i][1])
        order = ("x", "y") if i % 2 else ("y", "x")
        if stage == 0:
            copies = []
            for d in range(1, z_count):
                zz = lax.rem(z + z_count - d, z_count) if arriving else z
                block = rows_all.at[zz, x, y, c, :, cols]
                copies.append(
                    remote(block, block, gather_send.at[i, d], gather_recv.at[i, d], z_peer(d))
                )
            return copies
        axis = order[stage - 1] if stage < 3 else "c"
        xx = 1 - x if arriving and axis == "x" else x
        yy = 1 - y if arriving and axis == "y" else y
        cc = 1 - c if arriving and axis == "c" else c
        if stage == 1:
            block = rows_all.at[:, xx, yy, cc, :, cols]
        elif stage == 2 and axis == "x":
            block = rows_all.at[:, xx, :, cc, :, cols]
        elif stage == 2:
            block = rows_all.at[:, :, yy, cc, :, cols]
        else:
            block = rows_all.at[:, :, :, cc, :, cols]
        sem = z_count - 1 + stage
        return [
            remote(block, block, gather_send.at[i, sem], gather_recv.at[i, sem], partner[axis])
        ]

    chunks = len(gather_cuts)
    for tick in range(chunks + 4):
        for i in range(chunks):
            stage = tick - i
            if 1 <= stage <= 4:
                for copy in gather_copies(i, stage - 1, True):
                    copy.wait_recv()
            if 0 <= stage <= 3:
                for copy in gather_copies(i, stage, False):
                    copy.start()

    for load in loads:
        load.wait()
    quarter, wide = ext_ref.shape
    width = res_ref.shape[1]
    group = y_count * 2 * quarter

    @pl.loop(0, z_count * 2)
    def _(b):
        block = rows_all[b // 2, lax.rem(b, 2)].reshape(group, wide)
        rows = block[:, :width]
        gate_pre = jnp.dot(rows, gate_w[...], preferred_element_type=jnp.float32)
        up_pre = jnp.dot(rows, up_w[...], preferred_element_type=jnp.float32)
        hidden[b] = clamped_unit(gate_pre, up_pre).astype(jnp.bfloat16)
        lane = lax.broadcasted_iota(jnp.int32, (group, LANES), 1) % (LANES // 2)
        share = jnp.sum(
            jnp.where(lane == sp_me, block[:, width:].astype(jnp.float32), 0.0),
            axis=-1,
            keepdims=True,
        )
        shares[b] = jnp.broadcast_to(share, (group, LANES))

    def order_of(j):
        return ("x", "y") if j % 2 else ("y", "x")

    def reduce_copies(j, stage):
        axis = "c" if stage == 0 else order_of(j)[stage - 1] if stage < 3 else "z"
        if stage == 0:
            src, dst = parts.at[j, :, :, :, 1 - c], got_core.at[j]
        elif stage == 1 and axis == "y":
            src, dst = parts.at[j, :, :, 1 - y, c], got_first.at[j]
        elif stage == 1:
            src, dst = parts.at[j, :, 1 - x, :, c], got_first.at[j]
        elif stage == 2 and axis == "x":
            src, dst = parts.at[j, :, 1 - x, y, c], got_second.at[j]
        elif stage == 2:
            src, dst = parts.at[j, :, x, 1 - y, c], got_second.at[j]
        else:
            return [
                remote(
                    parts.at[j, lax.rem(z + d, z_count), x, y, c], got_z.at[j, d - 1],
                    reduce_send.at[j, 2 + d], reduce_recv.at[j, 2 + d], z_peer(d),
                )
                for d in range(1, z_count)
            ]
        return [
            remote(
                src, dst, reduce_send.at[j, stage], reduce_recv.at[j, stage], partner[axis]
            )
        ]

    def add(ours, theirs):
        return (ours.astype(jnp.float32) + theirs.astype(jnp.float32)).astype(jnp.bfloat16)

    def absorb(j, stage):
        for copy in reduce_copies(j, stage):
            copy.wait_recv()
        if stage == 3:
            cols = slice(reduce_cuts[j][0], reduce_cuts[j][0] + reduce_cuts[j][1])
            total = parts[j, z, x, y, c].astype(jnp.float32)
            for d in range(1, z_count):
                total = total + got_z[j, d - 1].astype(jnp.float32)
            out_ref[:, cols] = (res_ref[:, cols].astype(jnp.float32) + total).astype(jnp.bfloat16)
            return

        @pl.loop(0, z_count)
        def _(zz):
            if stage == 0:
                for xx in range(2):
                    for yy in range(y_count):
                        parts[j, zz, xx, yy, c] = add(
                            parts[j, zz, xx, yy, c], got_core[j, zz, xx, yy]
                        )
            elif stage == 1 and order_of(j)[0] == "y":
                for xx in range(2):
                    parts[j, zz, xx, y, c] = add(parts[j, zz, xx, y, c], got_first[j, zz, xx])
            elif stage == 1:
                for yy in range(y_count):
                    parts[j, zz, x, yy, c] = add(parts[j, zz, x, yy, c], got_first[j, zz, yy])
            else:
                parts[j, zz, x, y, c] = add(parts[j, zz, x, y, c], got_second[j, zz])

    pieces = len(reduce_cuts)
    for tick in range(pieces + 4):
        if tick < pieces:
            at, size = reduce_cuts[tick]

            @pl.loop(0, z_count * 2)
            def _(b):
                out = jnp.dot(
                    hidden[b], down_w[:, at : at + size], preferred_element_type=jnp.float32
                )
                out = (out * shares[b][:, 0:1]).astype(jnp.bfloat16)
                parts[tick, b // 2, lax.rem(b, 2)] = out.reshape(y_count, 2, quarter, size)

            reduce_copies(tick, 0)[0].start()
        for j in range(pieces):
            stage = tick - j
            if 1 <= stage <= 4:
                absorb(j, stage - 1)
                if stage < 4:
                    for copy in reduce_copies(j, stage):
                        copy.start()

    for i in range(chunks):
        for stage in range(4):
            for copy in gather_copies(i, stage, False):
                copy.wait_send()
    for j in range(pieces):
        for stage in range(4):
            for copy in reduce_copies(j, stage):
                copy.wait_send()


def cuts(total, pieces):
    tiles = total // LANES
    edges = [tiles * i // pieces * LANES for i in range(pieces + 1)]
    return [(edges[i], edges[i + 1] - edges[i]) for i in range(pieces)]


def expert_rows(extended, residual, gate_cols, up_cols, down_rows):
    z_count, y_count = lax.axis_size("sp") // 2, lax.axis_size("tp") // 2
    quarter, wide = extended.shape
    width, units = gate_cols.shape
    gather_cuts, reduce_cuts = cuts(wide, 4), cuts(width, 4)
    pieces, size = len(reduce_cuts), reduce_cuts[0][1]
    group = y_count * 2 * quarter
    vmem = pl.BlockSpec(memory_space=pltpu.VMEM)
    hbm = pl.BlockSpec(memory_space=pl.ANY)
    bf16 = jnp.bfloat16
    return pl.pallas_call(
        functools.partial(expert_kernel, z_count, y_count, gather_cuts, reduce_cuts),
        out_shape=jax.ShapeDtypeStruct((quarter, width), bf16),
        in_specs=[vmem, vmem, hbm, hbm, hbm],
        out_specs=vmem,
        scratch_shapes=[
            pltpu.VMEM((z_count, 2, y_count, 2, quarter, wide), bf16),
            pltpu.VMEM(gate_cols.shape, bf16),
            pltpu.VMEM(up_cols.shape, bf16),
            pltpu.VMEM(down_rows.shape, bf16),
            pltpu.VMEM((z_count * 2, group, units), bf16),
            pltpu.VMEM((z_count * 2, group, LANES), jnp.float32),
            pltpu.VMEM((pieces, z_count, 2, y_count, 2, quarter, size), bf16),
            pltpu.VMEM((pieces, z_count, 2, y_count, quarter, size), bf16),
            pltpu.VMEM((pieces, z_count, 2, quarter, size), bf16),
            pltpu.VMEM((pieces, z_count, quarter, size), bf16),
            pltpu.VMEM((pieces, z_count - 1, quarter, size), bf16),
            pltpu.SemaphoreType.DMA((3,)),
            pltpu.SemaphoreType.DMA,
            pltpu.SemaphoreType.DMA((len(gather_cuts), z_count + 3)),
            pltpu.SemaphoreType.DMA((len(gather_cuts), z_count + 3)),
            pltpu.SemaphoreType.DMA((pieces, z_count + 3)),
            pltpu.SemaphoreType.DMA((pieces, z_count + 3)),
        ],
        compiler_params=pltpu.CompilerParams(
            collective_id=1, has_side_effects=True, vmem_limit_bytes=56 << 20
        ),
        name="expert_rows",
    )(extended, residual, gate_cols, up_cols, down_rows)


def slot_ids(routes, capacity, experts):
    batch_size, rows_each, top_count = routes.shape
    flat_ids = routes.reshape(batch_size, rows_each * top_count)
    onehot = (flat_ids[:, :, None] == jnp.arange(experts, dtype=jnp.int32)[None, None, :]).astype(
        jnp.int32
    )
    earlier = jnp.cumsum(onehot, axis=1) - onehot
    rank_in = jnp.sum(earlier * onehot, axis=2)
    return (flat_ids * capacity + rank_in).reshape(batch_size, rows_each, top_count)


def dispatch_rows(slots, row_data, slot_total):
    chosen = jnp.any(slots[..., None] == jnp.arange(slot_total, dtype=jnp.int32), axis=2).astype(
        jnp.bfloat16
    )
    return jnp.einsum("brs,brd->bsd", chosen, row_data, preferred_element_type=jnp.float32).astype(
        jnp.bfloat16
    )


def on_device(
    residual_in,
    queries,
    key_rows,
    value_rows,
    out_gate,
    decay_logit,
    head_gain,
    w_out,
    ffn_gain,
    routing,
    route_weight,
    w_gate,
    w_up,
    w_down,
):
    tp_count = lax.axis_size("tp")
    experts = lax.axis_size("sp")
    quarter = residual_in.shape[0]
    top_count = routing.shape[1]
    model_width = residual_in.shape[1]
    capacity = 2 * routing.shape[0] * top_count // (tp_count * experts)
    slot_total = experts * capacity
    residual, extended = mix_rows(
        queries, key_rows, value_rows, out_gate, decay_logit, head_gain, w_out,
        ffn_gain, routing, route_weight, residual_in,
    )
    if capacity >= quarter and experts <= LANES // 2 and experts % 2 == 0 and tp_count == 4:
        return expert_rows(extended, residual, w_gate[0], w_up[0], w_down[0])
    normed = extended[:, :model_width]
    gate_cols = w_gate[0]
    up_cols = w_up[0]
    down_rows = w_down[0]
    own_routes = lax.dynamic_slice_in_dim(routing, lax.axis_index("tp") * quarter, quarter, 0)
    own_slots = slot_ids(own_routes[None], capacity, experts)[0]
    outgoing = dispatch_rows(own_slots[None], normed[None], slot_total)[0]
    arrived = lax.all_to_all(
        outgoing.reshape(experts, capacity, model_width),
        "sp",
        split_axis=0,
        concat_axis=0,
        tiled=True,
    )
    portion = lax.all_gather(arrived[None], "tp", axis=0, tiled=True)
    flat_rows = portion.reshape(-1, model_width)
    gate_pre = jnp.dot(flat_rows, gate_cols, preferred_element_type=jnp.float32)
    up_pre = jnp.dot(flat_rows, up_cols, preferred_element_type=jnp.float32)
    hidden_rows = clamped_unit(gate_pre, up_pre).astype(jnp.bfloat16)
    hidden = hidden_rows.reshape(portion.shape[:-1] + (gate_cols.shape[1],))
    portion = hidden
    partial_out = jnp.dot(
        portion.reshape(-1, hidden.shape[-1]), down_rows, preferred_element_type=jnp.float32
    ).astype(jnp.bfloat16)
    partial_out = lax.optimization_barrier(partial_out)
    summed = lax.psum_scatter(
        partial_out.astype(jnp.float32)
        .reshape(portion.shape[:-1] + (model_width,))
        .astype(jnp.bfloat16),
        "tp",
        scatter_dimension=0,
        tiled=True,
    ).astype(jnp.float32)
    returned = lax.all_to_all(
        summed[0].astype(jnp.bfloat16), "sp", split_axis=0, concat_axis=0, tiled=True
    )
    picked = jnp.take(
        returned.reshape(slot_total, model_width), own_slots.reshape(-1), axis=0
    ).reshape(quarter, top_count, model_width)
    routed = jnp.sum(picked.astype(jnp.float32) * route_weight[:, :, None], axis=1)
    return (residual.astype(jnp.float32) + routed).astype(jnp.bfloat16)


def solution(mesh):
    placed = (
        P(("sp", "tp"), None),
        P("sp", "tp"),
        P("sp", "tp"),
        P("sp", "tp"),
        P("sp", "tp"),
        P("sp", "tp"),
        P(),
        P(),
        P(),
        P("sp", None),
        P(("sp", "tp"), None),
        P("sp", None, "tp"),
        P("sp", None, "tp"),
        P("sp", "tp", None),
    )
    return jax.shard_map(
        on_device, mesh=mesh, in_specs=placed, out_specs=P(("sp", "tp"), None), check_vma=False
    )
```

```python
import jax
import jax.numpy as jnp
from jax import lax
from jax.experimental import pallas as pl
from jax.experimental.pallas import tpu as pltpu
from jax.sharding import PartitionSpec as P
import functools

DK = 64
DV = 128


DECAY_TEMP = 16.0
CLAMP_LIMIT = 7.0
SIGMOID_SLOPE = 1.702
NORM_EPS = 1e-06
EXACT_PRECISION = lax.Precision.HIGHEST


def clamped_unit(gate_pre, up_pre):
    gate_cut = jnp.minimum(gate_pre, CLAMP_LIMIT)
    up_cut = jnp.clip(up_pre, -CLAMP_LIMIT, CLAMP_LIMIT)
    return (up_cut + 1.0) * (gate_cut * jax.nn.sigmoid(SIGMOID_SLOPE * gate_cut))


MESH = pl.DeviceIdType.MESH
LANES = 128
SUB = 32
EXP_CAP = 64.0


def nt_dot(left, right):
    return lax.dot_general(
        left, right, (((1,), (1,)), ((), ())), preferred_element_type=jnp.float32
    )


def tn_dot(left, right):
    return lax.dot_general(
        left, right, (((0,), (0,)), ((), ())), preferred_element_type=jnp.float32
    )


def mix_kernel(
    sp_count, tp_count,
    q_ref, k_ref, v_ref, gate_ref, decay_ref, head_gain_ref, w_hbm, ffn_gain_ref,
    routing_ref, weight_ref, res_in_ref,
    res_ref, ext_ref,
    states, attended, mixed, mixed_in, w_vmem,
    w_sem, state_send, state_recv, mix_send, mix_recv,
):
    sp_me, tp_me = lax.axis_index("sp"), lax.axis_index("tp")
    barrier = pltpu.get_barrier_semaphore()

    @pl.loop(1, sp_count)
    def _(d):
        pl.semaphore_signal(
            barrier, inc=1, device_id={"sp": lax.rem(sp_me + d, sp_count)}, device_id_type=MESH
        )

    @pl.loop(1, tp_count)
    def _(d):
        pl.semaphore_signal(
            barrier, inc=1, device_id={"tp": lax.rem(tp_me + d, tp_count)}, device_id_type=MESH
        )

    w_copy = pltpu.make_async_copy(w_hbm, w_vmem, w_sem)
    w_copy.start()

    tokens, key_lanes = q_ref.shape
    value_lanes = v_ref.shape[1]
    head_count = key_lanes // DK
    lane_head = lax.broadcasted_iota(jnp.int32, (1, key_lanes), 1) // DK
    logit = decay_ref[...]
    log_decay = (jnp.minimum(logit, 0.0) - jnp.log1p(jnp.exp(-jnp.abs(logit)))) / DECAY_TEMP
    row_id = lax.broadcasted_iota(jnp.int32, (tokens, tokens), 0)
    col_id = lax.broadcasted_iota(jnp.int32, (tokens, tokens), 1)
    lower = (row_id >= col_id).astype(jnp.float32)
    cumulative = jnp.dot(
        lower, log_decay, precision=EXACT_PRECISION, preferred_element_type=jnp.float32
    )
    keys = k_ref[...].astype(jnp.float32)
    query = q_ref[...].astype(jnp.float32) * DK ** (-0.5)
    values = v_ref[...]
    ending = cumulative[tokens - 1 :, :]
    wide = tn_dot(values, (keys * jnp.exp(ending - cumulative)).astype(jnp.bfloat16))
    state = jnp.zeros((DV, key_lanes), jnp.float32)
    for h in range(head_count):
        state = jnp.where(lane_head == h, wide[h * DV : (h + 1) * DV, :], state)
    passing = jnp.exp(ending)
    passing_hi = passing.astype(jnp.bfloat16).astype(jnp.float32)
    tail_row = lax.broadcasted_iota(jnp.int32, (16, key_lanes), 0)
    tail = jnp.where(
        tail_row == 0, passing_hi, jnp.where(tail_row == 1, passing - passing_hi, 0.0)
    )
    states[sp_me, 0:DV, :] = state.astype(jnp.bfloat16)
    states[sp_me, DV : DV + 16, :] = tail.astype(jnp.bfloat16)

    pl.semaphore_wait(barrier, sp_count + tp_count - 2)

    def state_copy(slot, d):
        return pltpu.make_async_remote_copy(
            src_ref=states.at[slot],
            dst_ref=states.at[slot],
            send_sem=state_send.at[d],
            recv_sem=state_recv.at[slot],
            device_id={"sp": lax.rem(sp_me + d, sp_count)},
            device_id_type=MESH,
        )

    @pl.loop(1, sp_count)
    def _(d):
        state_copy(sp_me, d).start()

    for i in range(tokens // SUB):
        first = i * SUB
        reach = min(-(-(first + SUB) // LANES) * LANES, tokens)
        start = cumulative[first - 1 : first, :] if i else jnp.zeros((1, key_lanes), jnp.float32)
        q_sub = query[first : first + SUB] * jnp.exp(cumulative[first : first + SUB] - start)
        k_sub = keys[:reach] * jnp.exp(jnp.minimum(start - cumulative[:reach], EXP_CAP))
        stacked = jnp.concatenate(
            [jnp.where(lane_head == h, q_sub, 0.0) for h in range(head_count)], axis=0
        )
        scores = nt_dot(stacked.astype(jnp.bfloat16), k_sub.astype(jnp.bfloat16))
        at_row = lax.broadcasted_iota(jnp.int32, scores.shape, 0) % SUB + first
        at_col = lax.broadcasted_iota(jnp.int32, scores.shape, 1)
        scores = jnp.where(at_row >= at_col, scores, 0.0).astype(jnp.bfloat16)
        inner = jnp.dot(scores, values[:reach], preferred_element_type=jnp.float32)
        for h in range(head_count):
            attended[first : first + SUB, h * DV : (h + 1) * DV] = inner[
                h * SUB : (h + 1) * SUB, h * DV : (h + 1) * DV
            ]

    @pl.loop(1, sp_count)
    def _(d):
        state_copy(lax.rem(sp_me + d, sp_count), d).wait_recv()

    def absorb(j, incoming):
        decay = states[j, DV : DV + 16, :].astype(jnp.float32)
        total = decay[0:1, :] + decay[1:2, :]
        following = total * incoming + states[j, 0:DV, :].astype(jnp.float32)
        return jnp.where(j < sp_me, following, incoming)

    incoming = lax.fori_loop(
        0, sp_count, absorb, jnp.zeros((DV, key_lanes), jnp.float32)
    ).astype(jnp.bfloat16)
    query_dec = query * jnp.exp(cumulative)
    for h in range(head_count):
        cols = slice(h * DV, (h + 1) * DV)
        readout = nt_dot(jnp.where(lane_head == h, query_dec, 0.0).astype(jnp.bfloat16), incoming)
        head = attended[:, cols] + readout
        scale = lax.rsqrt(jnp.mean(head * head, axis=-1, keepdims=True) + NORM_EPS)
        opened = gate_ref[:, cols].astype(jnp.float32)
        opened = opened * jax.nn.sigmoid(opened)
        mixed[:, cols] = (head * scale * head_gain_ref[...].astype(jnp.float32) * opened).astype(
            jnp.bfloat16
        )

    rows = res_in_ref.shape[0]

    def mix_copy(block, slot, d):
        return pltpu.make_async_remote_copy(
            src_ref=mixed.at[pl.ds(pl.multiple_of(block * rows, rows), rows)],
            dst_ref=mixed_in.at[slot],
            send_sem=mix_send.at[d],
            recv_sem=mix_recv.at[slot],
            device_id={"tp": lax.rem(tp_me + d, tp_count)},
            device_id_type=MESH,
        )

    for d in range(1, tp_count):
        mix_copy(lax.rem(tp_me + d, tp_count), tp_me, d).start()

    lane = lax.broadcasted_iota(jnp.int32, (rows, LANES), 1)
    named = routing_ref[pl.ds(pl.multiple_of(tp_me * rows, rows), rows), :]
    share = jnp.zeros((rows, LANES), jnp.float32)
    for j in range(weight_ref.shape[1]):
        share = share + jnp.where(
            lane % (LANES // 2) == named[:, j : j + 1], weight_ref[:, j : j + 1], 0.0
        )
    share_hi = share.astype(jnp.bfloat16).astype(jnp.float32)
    width = res_in_ref.shape[1]
    ext_ref[:, width:] = jnp.where(lane < LANES // 2, share_hi, share - share_hi).astype(
        jnp.bfloat16
    )

    w_copy.wait()

    def w_rows(j):
        return w_vmem[pl.ds(pl.multiple_of(j * value_lanes, value_lanes), value_lanes), :]

    projected = jnp.dot(
        mixed[pl.ds(pl.multiple_of(tp_me * rows, rows), rows), :],
        w_rows(tp_me),
        preferred_element_type=jnp.float32,
    )
    for d in range(1, tp_count):
        slot = lax.rem(tp_me + d, tp_count)
        mix_copy(slot, slot, d).wait_recv()
        projected = projected + jnp.dot(
            mixed_in[slot], w_rows(slot), preferred_element_type=jnp.float32
        )
    residual = (res_in_ref[...].astype(jnp.float32) + projected).astype(jnp.bfloat16)
    res_ref[...] = residual
    wide_res = residual.astype(jnp.float32)
    inv = lax.rsqrt(jnp.mean(wide_res * wide_res, axis=-1, keepdims=True) + NORM_EPS)
    ext_ref[:, :width] = (wide_res * inv * ffn_gain_ref[...].astype(jnp.float32)).astype(
        jnp.bfloat16
    )

    @pl.loop(1, sp_count)
    def _(d):
        state_copy(sp_me, d).wait_send()

    for d in range(1, tp_count):
        mix_copy(lax.rem(tp_me + d, tp_count), tp_me, d).wait_send()


def mix_rows(
    queries, key_rows, value_rows, out_gate, decay_logit, head_gain, w_out,
    ffn_gain, routing, route_weight, residual_in,
):
    sp_count, tp_count = lax.axis_size("sp"), lax.axis_size("tp")
    rows, width = residual_in.shape
    tokens, key_lanes = queries.shape
    value_lanes = value_rows.shape[1]
    vmem = pl.BlockSpec(memory_space=pltpu.VMEM)
    return pl.pallas_call(
        functools.partial(mix_kernel, sp_count, tp_count),
        out_shape=(
            jax.ShapeDtypeStruct((rows, width), jnp.bfloat16),
            jax.ShapeDtypeStruct((rows, width + LANES), jnp.bfloat16),
        ),
        in_specs=[vmem] * 6 + [pl.BlockSpec(memory_space=pl.ANY)] + [vmem] * 4,
        out_specs=(vmem, vmem),
        scratch_shapes=[
            pltpu.VMEM((sp_count, DV + 16, key_lanes), jnp.bfloat16),
            pltpu.VMEM((tokens, value_lanes), jnp.float32),
            pltpu.VMEM((tokens, value_lanes), jnp.bfloat16),
            pltpu.VMEM((tp_count, rows, value_lanes), jnp.bfloat16),
            pltpu.VMEM(w_out.shape, jnp.bfloat16),
            pltpu.SemaphoreType.DMA,
            pltpu.SemaphoreType.DMA((sp_count,)),
            pltpu.SemaphoreType.DMA((sp_count,)),
            pltpu.SemaphoreType.DMA((tp_count,)),
            pltpu.SemaphoreType.DMA((tp_count,)),
        ],
        compiler_params=pltpu.CompilerParams(
            collective_id=0, has_side_effects=True, vmem_limit_bytes=40 << 20
        ),
        name="mix_rows",
    )(
        queries, key_rows, value_rows, out_gate, decay_logit, head_gain.reshape(1, -1), w_out,
        ffn_gain.reshape(1, -1), routing, route_weight, residual_in,
    )


def expert_kernel(
    z_count, y_count, gather_cuts, reduce_cuts,
    ext_ref, res_ref, gate_hbm, up_hbm, down_hbm, out_ref,
    rows_all, gate_w, up_w, down_w, hidden, shares, parts, got_core, got_first, got_second, got_z,
    w_sem, own_sem, gather_send, gather_recv, reduce_send, reduce_recv,
):
    sp_me, tp_me = lax.axis_index("sp"), lax.axis_index("tp")
    z, x = sp_me // 2, lax.rem(sp_me, 2)
    y, c = tp_me // 2, lax.rem(tp_me, 2)
    partner = {
        "x": {"sp": z * 2 + 1 - x},
        "y": {"tp": (1 - y) * 2 + c},
        "c": {"tp": y * 2 + 1 - c},
    }
    barrier = pltpu.get_barrier_semaphore()

    def z_peer(d):
        return {"sp": lax.rem(z + d, z_count) * 2 + x}

    for target in [z_peer(d) for d in range(1, z_count)] + list(partner.values()):
        pl.semaphore_signal(barrier, inc=1, device_id=target, device_id_type=MESH)
    loads = [
        pltpu.make_async_copy(src, dst, w_sem.at[i])
        for i, (src, dst) in enumerate(((gate_hbm, gate_w), (up_hbm, up_w), (down_hbm, down_w)))
    ]
    own = pltpu.make_async_copy(ext_ref, rows_all.at[z, x, y, c], own_sem)
    own.start()
    for load in loads:
        load.start()
    own.wait()
    pl.semaphore_wait(barrier, z_count + 2)

    def remote(src, dst, send, recv, target):
        return pltpu.make_async_remote_copy(
            src_ref=src, dst_ref=dst, send_sem=send, recv_sem=recv,
            device_id=target, device_id_type=MESH,
        )

    def gather_copies(i, stage, arriving):
        cols = pl.ds(gather_cuts[i][0], gather_cuts[i][1])
        order = ("x", "y") if i % 2 else ("y", "x")
        if stage == 0:
            copies = []
            for d in range(1, z_count):
                zz = lax.rem(z + z_count - d, z_count) if arriving else z
                block = rows_all.at[zz, x, y, c, :, cols]
                copies.append(
                    remote(block, block, gather_send.at[i, d], gather_recv.at[i, d], z_peer(d))
                )
            return copies
        axis = order[stage - 1] if stage < 3 else "c"
        xx = 1 - x if arriving and axis == "x" else x
        yy = 1 - y if arriving and axis == "y" else y
        cc = 1 - c if arriving and axis == "c" else c
        if stage == 1:
            block = rows_all.at[:, xx, yy, cc, :, cols]
        elif stage == 2 and axis == "x":
            block = rows_all.at[:, xx, :, cc, :, cols]
        elif stage == 2:
            block = rows_all.at[:, :, yy, cc, :, cols]
        else:
            block = rows_all.at[:, :, :, cc, :, cols]
        sem = z_count - 1 + stage
        return [
            remote(block, block, gather_send.at[i, sem], gather_recv.at[i, sem], partner[axis])
        ]

    chunks = len(gather_cuts)
    for tick in range(chunks // 2 + 4):
        for i in range(chunks):
            stage = tick - i // 2
            if 1 <= stage <= 4:
                for copy in gather_copies(i, stage - 1, True):
                    copy.wait_recv()
            if 0 <= stage <= 3:
                for copy in gather_copies(i, stage, False):
                    copy.start()

    for load in loads:
        load.wait()
    quarter, wide = ext_ref.shape
    width = res_ref.shape[1]
    group = y_count * 2 * quarter

    @pl.loop(0, z_count * 2)
    def _(b):
        block = rows_all[b // 2, lax.rem(b, 2)].reshape(group, wide)
        rows = block[:, :width]
        gate_pre = jnp.dot(rows, gate_w[...], preferred_element_type=jnp.float32)
        up_pre = jnp.dot(rows, up_w[...], preferred_element_type=jnp.float32)
        hidden[b] = clamped_unit(gate_pre, up_pre).astype(jnp.bfloat16)
        lane = lax.broadcasted_iota(jnp.int32, (group, LANES), 1) % (LANES // 2)
        share = jnp.sum(
            jnp.where(lane == sp_me, block[:, width:].astype(jnp.float32), 0.0),
            axis=-1,
            keepdims=True,
        )
        shares[b] = jnp.broadcast_to(share, (group, LANES))

    def order_of(j):
        return ("x", "y") if j % 2 else ("y", "x")

    def reduce_copies(j, stage):
        axis = "c" if stage == 0 else order_of(j)[stage - 1] if stage < 3 else "z"
        if stage == 0:
            src, dst = parts.at[j, :, :, :, 1 - c], got_core.at[j]
        elif stage == 1 and axis == "y":
            src, dst = parts.at[j, :, :, 1 - y, c], got_first.at[j]
        elif stage == 1:
            src, dst = parts.at[j, :, 1 - x, :, c], got_first.at[j]
        elif stage == 2 and axis == "x":
            src, dst = parts.at[j, :, 1 - x, y, c], got_second.at[j]
        elif stage == 2:
            src, dst = parts.at[j, :, x, 1 - y, c], got_second.at[j]
        else:
            return [
                remote(
                    parts.at[j, lax.rem(z + d, z_count), x, y, c], got_z.at[j, d - 1],
                    reduce_send.at[j, 2 + d], reduce_recv.at[j, 2 + d], z_peer(d),
                )
                for d in range(1, z_count)
            ]
        return [
            remote(
                src, dst, reduce_send.at[j, stage], reduce_recv.at[j, stage], partner[axis]
            )
        ]

    def add(ours, theirs):
        return (ours.astype(jnp.float32) + theirs.astype(jnp.float32)).astype(jnp.bfloat16)

    def absorb(j, stage):
        for copy in reduce_copies(j, stage):
            copy.wait_recv()
        if stage == 3:
            cols = slice(reduce_cuts[j][0], reduce_cuts[j][0] + reduce_cuts[j][1])
            total = parts[j, z, x, y, c].astype(jnp.float32)
            for d in range(1, z_count):
                total = total + got_z[j, d - 1].astype(jnp.float32)
            out_ref[:, cols] = (res_ref[:, cols].astype(jnp.float32) + total).astype(jnp.bfloat16)
            return

        @pl.loop(0, z_count)
        def _(zz):
            if stage == 0:
                for xx in range(2):
                    for yy in range(y_count):
                        parts[j, zz, xx, yy, c] = add(
                            parts[j, zz, xx, yy, c], got_core[j, zz, xx, yy]
                        )
            elif stage == 1 and order_of(j)[0] == "y":
                for xx in range(2):
                    parts[j, zz, xx, y, c] = add(parts[j, zz, xx, y, c], got_first[j, zz, xx])
            elif stage == 1:
                for yy in range(y_count):
                    parts[j, zz, x, yy, c] = add(parts[j, zz, x, yy, c], got_first[j, zz, yy])
            else:
                parts[j, zz, x, y, c] = add(parts[j, zz, x, y, c], got_second[j, zz])

    pieces = len(reduce_cuts)
    for tick in range(pieces // 2 + 4):
        for piece in range(2 * tick, min(2 * tick + 2, pieces)):
            at, size = reduce_cuts[piece]

            @pl.loop(0, z_count * 2)
            def _(b):
                out = jnp.dot(
                    hidden[b], down_w[:, at : at + size], preferred_element_type=jnp.float32
                )
                out = (out * shares[b][:, 0:1]).astype(jnp.bfloat16)
                parts[piece, b // 2, lax.rem(b, 2)] = out.reshape(y_count, 2, quarter, size)

            reduce_copies(piece, 0)[0].start()
        for j in range(pieces):
            stage = tick - j // 2
            if 1 <= stage <= 4:
                absorb(j, stage - 1)
                if stage < 4:
                    for copy in reduce_copies(j, stage):
                        copy.start()

    for i in range(chunks):
        for stage in range(4):
            for copy in gather_copies(i, stage, False):
                copy.wait_send()
    for j in range(pieces):
        for stage in range(4):
            for copy in reduce_copies(j, stage):
                copy.wait_send()


def cuts(total, pieces):
    tiles = total // LANES
    edges = [tiles * i // pieces * LANES for i in range(pieces + 1)]
    return [(edges[i], edges[i + 1] - edges[i]) for i in range(pieces)]


def expert_rows(extended, residual, gate_cols, up_cols, down_rows):
    z_count, y_count = lax.axis_size("sp") // 2, lax.axis_size("tp") // 2
    quarter, wide = extended.shape
    width, units = gate_cols.shape
    gather_cuts, reduce_cuts = cuts(wide, 8), cuts(width, 8)
    pieces, size = len(reduce_cuts), reduce_cuts[0][1]
    group = y_count * 2 * quarter
    vmem = pl.BlockSpec(memory_space=pltpu.VMEM)
    hbm = pl.BlockSpec(memory_space=pl.ANY)
    bf16 = jnp.bfloat16
    return pl.pallas_call(
        functools.partial(expert_kernel, z_count, y_count, gather_cuts, reduce_cuts),
        out_shape=jax.ShapeDtypeStruct((quarter, width), bf16),
        in_specs=[vmem, vmem, hbm, hbm, hbm],
        out_specs=vmem,
        scratch_shapes=[
            pltpu.VMEM((z_count, 2, y_count, 2, quarter, wide), bf16),
            pltpu.VMEM(gate_cols.shape, bf16),
            pltpu.VMEM(up_cols.shape, bf16),
            pltpu.VMEM(down_rows.shape, bf16),
            pltpu.VMEM((z_count * 2, group, units), bf16),
            pltpu.VMEM((z_count * 2, group, LANES), jnp.float32),
            pltpu.VMEM((pieces, z_count, 2, y_count, 2, quarter, size), bf16),
            pltpu.VMEM((pieces, z_count, 2, y_count, quarter, size), bf16),
            pltpu.VMEM((pieces, z_count, 2, quarter, size), bf16),
            pltpu.VMEM((pieces, z_count, quarter, size), bf16),
            pltpu.VMEM((pieces, z_count - 1, quarter, size), bf16),
            pltpu.SemaphoreType.DMA((3,)),
            pltpu.SemaphoreType.DMA,
            pltpu.SemaphoreType.DMA((len(gather_cuts), z_count + 3)),
            pltpu.SemaphoreType.DMA((len(gather_cuts), z_count + 3)),
            pltpu.SemaphoreType.DMA((pieces, z_count + 3)),
            pltpu.SemaphoreType.DMA((pieces, z_count + 3)),
        ],
        compiler_params=pltpu.CompilerParams(
            collective_id=1, has_side_effects=True, vmem_limit_bytes=56 << 20
        ),
        name="expert_rows",
    )(extended, residual, gate_cols, up_cols, down_rows)


def slot_ids(routes, capacity, experts):
    batch_size, rows_each, top_count = routes.shape
    flat_ids = routes.reshape(batch_size, rows_each * top_count)
    onehot = (flat_ids[:, :, None] == jnp.arange(experts, dtype=jnp.int32)[None, None, :]).astype(
        jnp.int32
    )
    earlier = jnp.cumsum(onehot, axis=1) - onehot
    rank_in = jnp.sum(earlier * onehot, axis=2)
    return (flat_ids * capacity + rank_in).reshape(batch_size, rows_each, top_count)


def dispatch_rows(slots, row_data, slot_total):
    chosen = jnp.any(slots[..., None] == jnp.arange(slot_total, dtype=jnp.int32), axis=2).astype(
        jnp.bfloat16
    )
    return jnp.einsum("brs,brd->bsd", chosen, row_data, preferred_element_type=jnp.float32).astype(
        jnp.bfloat16
    )


def on_device(
    residual_in,
    queries,
    key_rows,
    value_rows,
    out_gate,
    decay_logit,
    head_gain,
    w_out,
    ffn_gain,
    routing,
    route_weight,
    w_gate,
    w_up,
    w_down,
):
    tp_count = lax.axis_size("tp")
    experts = lax.axis_size("sp")
    quarter = residual_in.shape[0]
    top_count = routing.shape[1]
    model_width = residual_in.shape[1]
    capacity = 2 * routing.shape[0] * top_count // (tp_count * experts)
    slot_total = experts * capacity
    residual, extended = mix_rows(
        queries, key_rows, value_rows, out_gate, decay_logit, head_gain, w_out,
        ffn_gain, routing, route_weight, residual_in,
    )
    if capacity >= quarter and experts <= LANES // 2 and experts % 2 == 0 and tp_count == 4:
        return expert_rows(extended, residual, w_gate[0], w_up[0], w_down[0])
    normed = extended[:, :model_width]
    gate_cols = w_gate[0]
    up_cols = w_up[0]
    down_rows = w_down[0]
    own_routes = lax.dynamic_slice_in_dim(routing, lax.axis_index("tp") * quarter, quarter, 0)
    own_slots = slot_ids(own_routes[None], capacity, experts)[0]
    outgoing = dispatch_rows(own_slots[None], normed[None], slot_total)[0]
    arrived = lax.all_to_all(
        outgoing.reshape(experts, capacity, model_width),
        "sp",
        split_axis=0,
        concat_axis=0,
        tiled=True,
    )
    portion = lax.all_gather(arrived[None], "tp", axis=0, tiled=True)
    flat_rows = portion.reshape(-1, model_width)
    gate_pre = jnp.dot(flat_rows, gate_cols, preferred_element_type=jnp.float32)
    up_pre = jnp.dot(flat_rows, up_cols, preferred_element_type=jnp.float32)
    hidden_rows = clamped_unit(gate_pre, up_pre).astype(jnp.bfloat16)
    hidden = hidden_rows.reshape(portion.shape[:-1] + (gate_cols.shape[1],))
    portion = hidden
    partial_out = jnp.dot(
        portion.reshape(-1, hidden.shape[-1]), down_rows, preferred_element_type=jnp.float32
    ).astype(jnp.bfloat16)
    partial_out = lax.optimization_barrier(partial_out)
    summed = lax.psum_scatter(
        partial_out.astype(jnp.float32)
        .reshape(portion.shape[:-1] + (model_width,))
        .astype(jnp.bfloat16),
        "tp",
        scatter_dimension=0,
        tiled=True,
    ).astype(jnp.float32)
    returned = lax.all_to_all(
        summed[0].astype(jnp.bfloat16), "sp", split_axis=0, concat_axis=0, tiled=True
    )
    picked = jnp.take(
        returned.reshape(slot_total, model_width), own_slots.reshape(-1), axis=0
    ).reshape(quarter, top_count, model_width)
    routed = jnp.sum(picked.astype(jnp.float32) * route_weight[:, :, None], axis=1)
    return (residual.astype(jnp.float32) + routed).astype(jnp.bfloat16)


def solution(mesh):
    placed = (
        P(("sp", "tp"), None),
        P("sp", "tp"),
        P("sp", "tp"),
        P("sp", "tp"),
        P("sp", "tp"),
        P("sp", "tp"),
        P(),
        P(),
        P(),
        P("sp", None),
        P(("sp", "tp"), None),
        P("sp", None, "tp"),
        P("sp", None, "tp"),
        P("sp", "tp", None),
    )
    return jax.shard_map(
        on_device, mesh=mesh, in_specs=placed, out_specs=P(("sp", "tp"), None), check_vma=False
    )
```
